32 devices in a mesh: sp: 16 (over z, y, x), tp: 2 (over core).
Axes of the slice: x: 2, y: 2, z: 4, core: 2. Of those that a mesh axis runs over, the one named last changes fastest.
Arguments:
- hidden_in: bfloat16 [4096, 2048], P('sp'), may hold values from -16 to 16
- query_one: bfloat16 [2048, 512], P(None, 'tp'), may hold values from -0.13258252 to 0.13258252
- query_two: bfloat16 [2048, 512], P(None, 'tp'), may hold values from -0.13258252 to 0.13258252
- key_one: bfloat16 [2048, 512], P(None, 'tp'), may hold values from -0.13258252 to 0.13258252
- key_two: bfloat16 [2048, 512], P(None, 'tp'), may hold values from -0.13258252 to 0.13258252
- value_proj: bfloat16 [2048, 1024], P(None, 'tp'), may hold values from -0.125 to 0.125
- lambdas: float32 [8], P('tp'), may hold values from 0.3 to 0.8
- norm_gain: float32 [128], replicated, may hold values from 0.1 to 1.9
- out_proj: bfloat16 [1024, 2048], P('tp'), may hold values from -0.1875 to 0.1875
Outputs:
- attended: bfloat16 [4096, 2048], P('sp')
The draws below stay inside these ranges and needn't reach their ends.
All inputs are finite; a program needn't handle non-finite values.
Results may differ from the reference program's by a relative error of at most 0.015.
Values may be sent and summed in bfloat16 or wider, within the bound.
A program may use at most 64 MiB of HBM per device.

```python
import math
import jax
import jax.numpy as jnp
from jax import lax

D = 2048
HEADS = 8
HEAD_QK = 64
HEAD_V = 128
TOK_DEV = 256
TOKENS = 4096
N_TP = 2


def draw_hidden_in(key, part):
    blocks = TOKENS // TOK_DEV
    noise_key = jax.random.fold_in(key, 101)
    shift_key = jax.random.fold_in(key, 102)
    offsets = 0.6 * jax.random.normal(shift_key, (blocks, 1, D), jnp.float32)
    base = 0.8 * jax.random.normal(noise_key, (blocks, TOK_DEV, D), jnp.float32)
    field = base + offsets
    return jnp.clip(field.reshape(TOKENS, D), -16.0, 16.0).astype(jnp.bfloat16)


def plain_weight(key, salt):
    base = jax.random.normal(jax.random.fold_in(key, salt), (D, HEADS * HEAD_QK), jnp.float32)
    return jnp.clip(base, -6.0, 6.0) * D ** (-0.5)


def draw_query_one(key, part):
    return plain_weight(key, 201).astype(jnp.bfloat16)


def draw_query_two(key, part):
    return plain_weight(key, 301).astype(jnp.bfloat16)


def draw_key_one(key, part):
    return plain_weight(key, 211).astype(jnp.bfloat16)


def draw_key_two(key, part):
    return plain_weight(key, 311).astype(jnp.bfloat16)


def shard_levels(rng, dims, split, least, high):
    loudness = 1.0
    for dim, blocks in split:
        draws = jax.random.uniform(jax.random.fold_in(jax.random.fold_in(rng, 6), dim), (blocks,), jnp.float32, least / len(split), high / len(split))
        loudness = loudness * jnp.repeat(jnp.exp(draws), dims[dim] // blocks).reshape((-1,) + (1,) * (len(dims) - 1 - dim))
    return loudness


def scatter_about(key, dims, spread, bound, split=(), held_as=jnp.bfloat16):
    array = jax.random.normal(key, dims, jnp.float32) * spread
    if len(split) > 0:
        array = shard_levels(key, dims, split, -0.22, 0.18) * array
    return jnp.clip(array, min=-bound, max=bound).astype(held_as)


def setup_inputs(seed: int = 0) -> dict:
    key_list = jax.random.split(jax.random.key(seed), 10)
    hidden_in = draw_hidden_in(jax.random.fold_in(key_list[9], 71), 0)
    query_one = draw_query_one(jax.random.fold_in(key_list[9], 71), 0)
    query_two = draw_query_two(jax.random.fold_in(key_list[9], 71), 0)
    key_one = draw_key_one(jax.random.fold_in(key_list[9], 71), 0)
    key_two = draw_key_two(jax.random.fold_in(key_list[9], 71), 0)
    value_proj = scatter_about(key_list[5], (D, HEADS * HEAD_V), D ** -0.5, 0.125, ((1, 2),))
    lambdas = jnp.clip(0.3 + 0.5 * jax.random.uniform(key_list[6], (HEADS,), jnp.float32) ** shard_levels(key_list[6], (HEADS,), ((0, 2),), -0.2, 0.2), 0.3, 0.8)
    norm_gain = jnp.clip(1.0 + 0.18 * jax.random.normal(key_list[7], (HEAD_V,), jnp.float32), 0.1, 1.9)
    out_proj = scatter_about(key_list[8], (HEADS * HEAD_V, D), (HEADS * HEAD_V) ** -0.5, 0.1875, ((0, 2),))
    return {"hidden_in": hidden_in, "query_one": query_one, "query_two": query_two, "key_one": key_one, "key_two": key_two, "value_proj": value_proj, "lambdas": lambdas, "norm_gain": norm_gain, "out_proj": out_proj}


epsilon = 1e-06
masked_score = -1e+30

def reference(hidden_in, query_one, query_two, key_one, key_two, value_proj, lambdas, norm_gain, out_proj):

    def project(weight, width):
        product = jnp.dot(hidden_in, weight, preferred_element_type=jnp.float32)
        return product.astype(jnp.bfloat16).reshape(TOKENS, HEADS, width)
    query_a = project(query_one, HEAD_QK)
    query_b = project(query_two, HEAD_QK)
    keys_a = project(key_one, HEAD_QK).astype(jnp.float32)
    keys_b = project(key_two, HEAD_QK).astype(jnp.float32)
    value_rows = project(value_proj, HEAD_V).astype(jnp.float32)
    score_scale = 1.75 * HEAD_QK ** (-0.5)
    key_pos = jnp.arange(TOKENS, dtype=jnp.int32)
    query_rows = math.gcd(TOKENS, 512)

    def one_block(block_index):
        begin = block_index * query_rows
        row_pos = begin + jnp.arange(query_rows, dtype=jnp.int32)
        allowed = key_pos[None, :] <= row_pos[:, None]

        def attend(queries, keys):
            chosen = lax.dynamic_slice_in_dim(queries, begin, query_rows, 0).astype(jnp.float32)
            scores = jnp.einsum('qhd,khd->hqk', chosen, keys) * score_scale
            scores = jnp.where(allowed[None], scores, masked_score)
            highest = lax.optimization_barrier(jnp.max(scores, axis=-1, keepdims=True))
            expos = jnp.where(allowed[None], jnp.exp(scores - highest), 0.0)
            summed = lax.optimization_barrier(jnp.sum(expos, axis=-1))
            rounded = lax.optimization_barrier(expos.astype(jnp.bfloat16))
            accum = jnp.einsum('hqk,khe->hqe', rounded.astype(jnp.float32), value_rows)
            return accum / summed[..., None]
        mixed_out = attend(query_a, keys_a) - lambdas[:, None, None] * attend(query_b, keys_b)
        scale_rows = lax.rsqrt(lax.optimization_barrier(jnp.mean(mixed_out * mixed_out, axis=-1, keepdims=True)) + epsilon)
        normed = (mixed_out * scale_rows * norm_gain).astype(jnp.bfloat16)
        return jnp.transpose(normed, (1, 0, 2)).reshape(query_rows, HEADS * HEAD_V)
    normed = lax.map(one_block, jnp.arange(TOKENS // query_rows, dtype=jnp.int32))
    normed = normed.reshape(TOKENS, HEADS * HEAD_V)
    group_cols = HEADS * HEAD_V // N_TP
    summed = jnp.zeros((TOKENS, D), jnp.float32)
    for group_index in range(N_TP):
        lower = group_index * group_cols
        part = jnp.dot(normed[:, lower:lower + group_cols], out_proj[lower:lower + group_cols], preferred_element_type=jnp.float32).astype(jnp.bfloat16)
        part = lax.optimization_barrier(part)
        summed = summed + part.astype(jnp.float32)
    return summed.astype(jnp.bfloat16)
```

```python
import math

import jax
import jax.numpy as jnp
from jax import lax
from jax.experimental import pallas as pl
from jax.experimental.pallas import tpu as pltpu
from jax.sharding import PartitionSpec as P

epsilon = 1e-06
masked_score = -1e30


def shards(
    hidden_in, query_one, query_two, key_one, key_two, value_proj, lambdas, norm_gain, out_proj
):
    heads_dev = lambdas.shape[0]
    head_qk = query_one.shape[1] // heads_dev
    head_v = value_proj.shape[1] // heads_dev
    width_q = heads_dev * head_qk
    score_scale = 1.75 * head_qk ** (-0.5)
    joined = jnp.concatenate((query_one, query_two, key_one, key_two, value_proj), axis=1)
    projected = jnp.dot(hidden_in, joined, preferred_element_type=jnp.float32).astype(jnp.bfloat16)
    tok_rows = projected.shape[0]
    key_values = projected[:, 2 * width_q :]
    my_index = lax.axis_index("sp")
    offset = my_index * tok_rows
    query_sets = (projected[:, : 2 * width_q],)
    position_sets = (offset + jnp.arange(tok_rows, dtype=jnp.int32),)
    groups = []
    for query_rows, positions in zip(query_sets, position_sets):
        group_rows = query_rows.shape[0]
        query_a = query_rows[:, :width_q].reshape(group_rows, heads_dev, head_qk)
        query_b = query_rows[:, width_q:].reshape(group_rows, heads_dev, head_qk)
        groups.append((query_a, query_b, positions, positions[group_rows - 1]))

    def one_map(queries, keys, value_rows, allowed, running_max, running_sum, accum):
        scores = (
            jnp.einsum("qhd,khd->hqk", queries, keys, preferred_element_type=jnp.float32)
            * score_scale
        )
        scores = jnp.where(allowed[None], scores, masked_score)
        new_max = jnp.maximum(running_max, jnp.max(scores, axis=-1))
        rescale = jnp.exp(running_max - new_max)
        weights = jnp.where(allowed[None], jnp.exp(scores - new_max[..., None]), 0.0)
        new_sum = running_sum * rescale + jnp.sum(weights, axis=-1)
        added = jnp.einsum(
            "hqk,khe->hqe",
            weights.astype(jnp.bfloat16),
            value_rows,
            preferred_element_type=jnp.float32,
        )
        return (new_max, new_sum, accum * rescale[..., None] + added)

    def absorb(group_state, group, kblock, kstart):
        query_a, query_b, positions, last_pos = group
        block_rows = kblock.shape[0]
        k_pos = kstart + jnp.arange(block_rows, dtype=jnp.int32)
        allowed = k_pos[None, :] <= positions[:, None]
        keys_a = kblock[:, :width_q].reshape(block_rows, heads_dev, head_qk)
        keys_b = kblock[:, width_q : 2 * width_q].reshape(block_rows, heads_dev, head_qk)
        value_rows = kblock[:, 2 * width_q :].reshape(block_rows, heads_dev, head_v)
        first_map = one_map(query_a, keys_a, value_rows, allowed, *group_state[:3])
        second_map = one_map(query_b, keys_b, value_rows, allowed, *group_state[3:])
        return first_map + second_map

    group = groups[0]
    group_rows = group[0].shape[0]
    start_max = jnp.full((heads_dev, group_rows), masked_score, jnp.float32)
    start_sum = jnp.zeros((heads_dev, group_rows), jnp.float32)
    start_acc = jnp.zeros((heads_dev, group_rows, head_v), jnp.float32)
    initial_list = [(start_max, start_sum, start_acc, start_max, start_sum, start_acc)]
    initial = tuple(initial_list)
    softmax_state = initial
    kv_piece = lax.all_gather(key_values, "sp", axis=0, tiled=True)
    piece_rows = kv_piece.shape[0]
    block_rows = math.gcd(piece_rows, 512)
    block_count = piece_rows // block_rows
    stacked = kv_piece.reshape(block_count, block_rows, kv_piece.shape[1])

    def absorb_step(carried, blocks_in):
        kblock, block_index = blocks_in
        kstart = block_index * block_rows
        renewed = []
        for group, group_state in zip(groups, carried):
            renewed.append(
                lax.cond(
                    kstart <= group[3],
                    lambda inner, group=group: absorb(inner, group, kblock, kstart),
                    lambda inner: inner,
                    group_state,
                )
            )
        return (tuple(renewed), None)

    softmax_state, _ = lax.scan(
        absorb_step, softmax_state, (stacked, jnp.arange(block_count, dtype=jnp.int32))
    )
    normed_sets = []
    for group_state in softmax_state:
        out_a = group_state[2] / group_state[1][..., None]
        out_b = group_state[5] / group_state[4][..., None]
        mixed_out = out_a - lambdas[:, None, None] * out_b
        scale_rows = lax.rsqrt(jnp.mean(mixed_out * mixed_out, axis=-1, keepdims=True) + epsilon)
        normed = (mixed_out * scale_rows * norm_gain).astype(jnp.bfloat16)
        group_rows = normed.shape[1]
        normed_sets.append(jnp.transpose(normed, (1, 0, 2)).reshape(group_rows, heads_dev * head_v))
    normed_all = normed_sets[0]
    partial_value = jnp.dot(normed_all, out_proj, preferred_element_type=jnp.float32)
    result = lax.psum(partial_value.astype(jnp.bfloat16), "tp")
    return result


MESH = pl.DeviceIdType.MESH
PLANE = 4


def fused_kernel(
    groups,
    score_scale,
    hidden_hbm,
    q1_hbm,
    q2_hbm,
    k1_hbm,
    k2_hbm,
    v_hbm,
    lam_ref,
    gain_ref,
    wo_hbm,
    out_ref,
    hid,
    wq1,
    wq2,
    wk1,
    wk2,
    wv,
    wo,
    kv_out,
    q_out,
    kv_all,
    q_all,
    n_out,
    n_all,
    load_sem,
    wo_send,
    wo_recv,
    kv_send,
    kv_recv,
    q_send,
    q_recv,
    x_send,
    x_recv,
    y_send,
    y_recv,
    f_send,
    f_recv,
    n_send,
    n_recv,
):
    me = lax.axis_index("sp")
    core = lax.axis_index("tp")
    plane = me // PLANE
    spot = lax.rem(me, PLANE)
    x_spot = spot + 1 - 2 * lax.rem(spot, 2)
    y_spot = spot + 2 - 4 * (spot // 2)
    rows = hid.shape[0]
    qk = q1_hbm.shape[1] // groups
    width = 2 * qk

    def load(index, src, dst):
        return pltpu.make_async_copy(src, dst, load_sem.at[index])

    loads = [
        load(0, hidden_hbm, hid),
        load(1, k1_hbm, wk1),
        load(2, k2_hbm, wk2),
        load(3, v_hbm, wv),
        load(4, q1_hbm, wq1),
        load(5, q2_hbm, wq2),
        load(6, wo_hbm, wo.at[core]),
    ]
    for item in loads:
        item.start()

    barrier = pltpu.get_barrier_semaphore()

    def greet(index, tp_index):
        pl.semaphore_signal(
            barrier, inc=1, device_id=(index, tp_index), device_id_type=MESH
        )

    for step in range(1, groups):
        other = lax.rem(plane + step, groups) * PLANE + spot
        greet(other, core)
        greet(other, 1 - core)
    greet(me, 1 - core)
    greet(plane * PLANE + x_spot, core)
    greet(plane * PLANE + y_spot, core)
    pl.semaphore_wait(barrier, 2 * (groups - 1) + 3)

    def send(src, dst, send_sem, recv_sem, index, tp_index):
        return pltpu.make_async_remote_copy(
            src_ref=src,
            dst_ref=dst,
            send_sem=send_sem,
            recv_sem=recv_sem,
            device_id=(index, tp_index),
            device_id_type=MESH,
        )

    loads[0].wait()
    pending = []

    def project(weight_ref):
        return jnp.dot(hid[...], weight_ref[...], preferred_element_type=jnp.float32)

    loads[1].wait()
    first = project(wk1).astype(jnp.bfloat16)
    loads[2].wait()
    second = project(wk2).astype(jnp.bfloat16)
    for head in range(groups):
        cut = slice(head * qk, (head + 1) * qk)
        kv_out[head, :, :width] = jnp.concatenate((first[:, cut], second[:, cut]), axis=1)
    loads[3].wait()
    head_v = v_hbm.shape[1] // groups
    for head in range(groups):
        cut = slice(head * head_v, (head + 1) * head_v)
        kv_out[head, :, width:] = jnp.dot(
            hid[...], wv[:, cut], preferred_element_type=jnp.float32
        ).astype(jnp.bfloat16)
    kv_all[me] = kv_out[plane]
    kv_copies = [None]
    for step in range(1, groups):
        target = lax.rem(plane + step, groups)
        copy = send(
            kv_out.at[target],
            kv_all.at[me],
            kv_send.at[step],
            kv_recv.at[step],
            target * PLANE + spot,
            core,
        )
        copy.start()
        kv_copies.append(copy)

    def from_plane(step):
        return lax.rem(plane - step + groups, groups)

    def spread(step):
        block = from_plane(step) * PLANE + spot
        for sems, where in (((x_send, x_recv), x_spot), ((y_send, y_recv), y_spot)):
            copy = send(
                kv_all.at[block],
                kv_all.at[block],
                sems[0].at[step],
                sems[1].at[step],
                plane * PLANE + where,
                core,
            )
            copy.start()
            pending.append(copy)

    def arrived(recv_sem, block):
        pltpu.make_async_copy(kv_all.at[block], kv_all.at[block], recv_sem).wait()

    def relay(step):
        x_block = from_plane(step) * PLANE + x_spot
        y_block = from_plane(step) * PLANE + y_spot
        arrived(x_recv.at[step], x_block)
        arrived(y_recv.at[step], y_block)
        block, where = (x_block, y_spot) if step % 2 == 0 else (y_block, x_spot)
        copy = send(
            kv_all.at[block],
            kv_all.at[block],
            f_send.at[step],
            f_recv.at[step],
            plane * PLANE + where,
            core,
        )
        copy.start()
        pending.append(copy)

    spread(0)

    loads[4].wait()
    first = (project(wq1) * score_scale).astype(jnp.bfloat16)
    loads[5].wait()
    second = (project(wq2) * score_scale).astype(jnp.bfloat16)
    for head in range(groups):
        cut = slice(head * qk, (head + 1) * qk)
        q_out[head] = jnp.concatenate((first[:, cut], second[:, cut]), axis=1)
    q_all[plane] = q_out[plane]
    q_copies = [None]
    for step in range(1, groups):
        target = lax.rem(plane + step, groups)
        copy = send(
            q_out.at[target],
            q_all.at[plane],
            q_send.at[step],
            q_recv.at[step],
            target * PLANE + spot,
            core,
        )
        copy.start()
        q_copies.append(copy)
    loads[6].wait()
    wo_copy = send(wo.at[core], wo.at[core], wo_send, wo_recv, me, 1 - core)
    wo_copy.start()

    for step in range(1, groups):
        arrived(kv_recv.at[step], from_plane(step) * PLANE + spot)
        spread(step)
        relay(step - 1)
    relay(groups - 1)
    for step in range(groups):
        arrived(f_recv.at[step], from_plane(step) * PLANE + (PLANE - 1 - spot))
    for step in range(1, groups):
        source = from_plane(step)
        pltpu.make_async_copy(q_all.at[source], q_all.at[source], q_recv.at[step]).wait()

    tile = ROW_TILE
    chunk = PLANE * rows
    lane = lax.broadcasted_iota(jnp.int32, (tile, width), 1)
    lam = lam_ref[plane]
    gain = gain_ref[...]

    def attend_tile(group, part):
        begin = pl.multiple_of(part * tile, tile)
        queries = q_all[group, pl.ds(begin, tile), :]
        zero = jnp.zeros_like(queries)
        both = jnp.concatenate(
            (jnp.where(lane < qk, queries, zero), jnp.where(lane >= qk, queries, zero)), axis=0
        )

        def absorb(key_group, carry, diagonal):
            running_max, running_sum, accum = carry
            block = kv_all[pl.ds(key_group * PLANE, PLANE)].reshape(chunk, width + head_v)
            scores = lax.dot_general(
                both,
                block[:, :width],
                (((1,), (1,)), ((), ())),
                preferred_element_type=jnp.float32,
            )
            if diagonal:
                q_pos = spot * rows + begin + lax.rem(
                    lax.broadcasted_iota(jnp.int32, (2 * tile, chunk), 0), tile
                )
                k_pos = lax.broadcasted_iota(jnp.int32, (2 * tile, chunk), 1)
                scores = jnp.where(k_pos <= q_pos, scores, masked_score)
            new_max = jnp.maximum(running_max, jnp.max(scores, axis=-1, keepdims=True))
            weights = jnp.exp2(scores - new_max)
            rescale = jnp.exp2(running_max - new_max)
            new_sum = running_sum * rescale + jnp.sum(weights, axis=-1, keepdims=True)
            added = jnp.dot(
                weights.astype(jnp.bfloat16),
                block[:, width:],
                preferred_element_type=jnp.float32,
            )
            return (new_max, new_sum, accum * rescale + added)

        carry = (
            jnp.full((2 * tile, 1), masked_score, jnp.float32),
            jnp.zeros((2 * tile, 1), jnp.float32),
            jnp.zeros((2 * tile, head_v), jnp.float32),
        )
        carry = absorb(group, carry, True)
        carry = lax.fori_loop(0, group, lambda k, c: absorb(k, c, False), carry)
        heads_out = carry[2] / carry[1]
        mixed = heads_out[:tile] - lam * heads_out[tile:]
        scale_rows = lax.rsqrt(jnp.mean(mixed * mixed, axis=-1, keepdims=True) + epsilon)
        n_out[group, pl.ds(begin, tile), :] = (mixed * scale_rows * gain).astype(jnp.bfloat16)

    def normed_copy(group, tp_index):
        return send(
            n_out.at[group],
            n_all.at[core, plane],
            n_send.at[group, tp_index],
            n_recv.at[core, plane],
            group * PLANE + spot,
            tp_index,
        )

    def attend_group(turn, _):
        group = groups - 1 - turn
        lax.fori_loop(0, rows // tile, lambda t, c: (attend_tile(group, t), c)[1], 0)
        normed_copy(group, 1 - core).start()

        @pl.when(group != plane)
        def _():
            normed_copy(group, core).start()

        @pl.when(group == plane)
        def _():
            n_all[core, plane] = n_out[plane]

        return 0

    lax.fori_loop(0, groups, attend_group, 0)

    wo_copy.wait_send()
    pltpu.make_async_copy(wo.at[1 - core], wo.at[1 - core], wo_recv).wait()
    for tp_index in range(2):
        for head in range(groups):

            @pl.when(jnp.logical_or(head != plane, tp_index != core))
            def _():
                slot = n_all.at[tp_index, head]
                pltpu.make_async_copy(slot, slot, n_recv.at[tp_index, head]).wait()

    halves = [
        jnp.concatenate([n_all[tp_index, head] for head in range(groups)], axis=1)
        for tp_index in range(2)
    ]

    def out_tile(index, _):
        columns = pl.ds(pl.multiple_of(index * OUT_TILE, OUT_TILE), OUT_TILE)
        total = None
        for tp_index in range(2):
            part = jnp.dot(
                halves[tp_index], wo[tp_index, :, columns], preferred_element_type=jnp.float32
            )
            part = part.astype(jnp.bfloat16).astype(jnp.float32)
            total = part if total is None else total + part
        out_ref[:, columns] = total.astype(jnp.bfloat16)
        return 0

    lax.fori_loop(0, out_ref.shape[1] // OUT_TILE, out_tile, 0)

    for copy in pending:
        copy.wait_send()
    for step in range(1, groups):
        kv_copies[step].wait_send()
        q_copies[step].wait_send()
    for group in range(groups):
        normed_copy(group, 1 - core).wait_send()

        @pl.when(group != plane)
        def _():
            normed_copy(group, core).wait_send()


ROW_TILE = 128
OUT_TILE = 256


def fused_shards(
    hidden_in, query_one, query_two, key_one, key_two, value_proj, lambdas, norm_gain, out_proj
):
    groups = lambdas.shape[0]
    rows, depth = hidden_in.shape
    head_qk = query_one.shape[1] // groups
    head_v = value_proj.shape[1] // groups
    width = 2 * head_qk
    blocks = groups * PLANE
    columns = out_proj.shape[1]
    score_scale = 1.75 * head_qk ** (-0.5) * math.log2(math.e)
    bf16 = jnp.bfloat16
    dma = pltpu.SemaphoreType.DMA
    hbm = pl.BlockSpec(memory_space=pl.ANY)
    vmem = pl.BlockSpec(memory_space=pltpu.VMEM)
    smem = pl.BlockSpec(memory_space=pltpu.SMEM)

    def body(*refs):
        fused_kernel(groups, score_scale, *refs)

    return pl.pallas_call(
        body,
        name="fused_attention",
        out_shape=jax.ShapeDtypeStruct((rows, columns), bf16),
        in_specs=[hbm] * 6 + [smem, vmem, hbm],
        out_specs=vmem,
        scratch_shapes=[
            pltpu.VMEM(hidden_in.shape, bf16),
            pltpu.VMEM(query_one.shape, bf16),
            pltpu.VMEM(query_two.shape, bf16),
            pltpu.VMEM(key_one.shape, bf16),
            pltpu.VMEM(key_two.shape, bf16),
            pltpu.VMEM(value_proj.shape, bf16),
            pltpu.VMEM((2,) + out_proj.shape, bf16),
            pltpu.VMEM((groups, rows, width + head_v), bf16),
            pltpu.VMEM((groups, rows, width), bf16),
            pltpu.VMEM((blocks, rows, width + head_v), bf16),
            pltpu.VMEM((groups, rows, width), bf16),
            pltpu.VMEM((groups, rows, head_v), bf16),
            pltpu.VMEM((2, groups, rows, head_v), bf16),
            dma((7,)),
            dma,
            dma,
        ]
        + [dma((groups,))] * 10
        + [dma((groups, 2)), dma((2, groups))],
        compiler_params=pltpu.CompilerParams(
            collective_id=0, has_side_effects=True, vmem_limit_bytes=60 * 1024 * 1024
        ),
    )(
        hidden_in,
        query_one,
        query_two,
        key_one,
        key_two,
        value_proj,
        lambdas,
        norm_gain.reshape(1, head_v),
        out_proj,
    )


def solution(mesh):
    placed = (
        P("sp", None),
        P(None, "tp"),
        P(None, "tp"),
        P(None, "tp"),
        P(None, "tp"),
        P(None, "tp"),
        P("tp"),
        P(),
        P("tp", None),
    )

    def body(*args):
        groups = args[6].shape[0]
        split = groups * PLANE == mesh.shape["sp"] and mesh.shape["tp"] == 2
        return (fused_shards if split else shards)(*args)

    return jax.shard_map(
        body, mesh=mesh, in_specs=placed, out_specs=P("sp", None), check_vma=False
    )
```

```python
import math

import jax
import jax.numpy as jnp
from jax import lax
from jax.experimental import pallas as pl
from jax.experimental.pallas import tpu as pltpu
from jax.sharding import PartitionSpec as P

epsilon = 1e-06
masked_score = -1e30


def shards(
    hidden_in, query_one, query_two, key_one, key_two, value_proj, lambdas, norm_gain, out_proj
):
    heads_dev = lambdas.shape[0]
    head_qk = query_one.shape[1] // heads_dev
    head_v = value_proj.shape[1] // heads_dev
    width_q = heads_dev * head_qk
    score_scale = 1.75 * head_qk ** (-0.5)
    joined = jnp.concatenate((query_one, query_two, key_one, key_two, value_proj), axis=1)
    projected = jnp.dot(hidden_in, joined, preferred_element_type=jnp.float32).astype(jnp.bfloat16)
    tok_rows = projected.shape[0]
    key_values = projected[:, 2 * width_q :]
    my_index = lax.axis_index("sp")
    offset = my_index * tok_rows
    query_sets = (projected[:, : 2 * width_q],)
    position_sets = (offset + jnp.arange(tok_rows, dtype=jnp.int32),)
    groups = []
    for query_rows, positions in zip(query_sets, position_sets):
        group_rows = query_rows.shape[0]
        query_a = query_rows[:, :width_q].reshape(group_rows, heads_dev, head_qk)
        query_b = query_rows[:, width_q:].reshape(group_rows, heads_dev, head_qk)
        groups.append((query_a, query_b, positions, positions[group_rows - 1]))

    def one_map(queries, keys, value_rows, allowed, running_max, running_sum, accum):
        scores = (
            jnp.einsum("qhd,khd->hqk", queries, keys, preferred_element_type=jnp.float32)
            * score_scale
        )
        scores = jnp.where(allowed[None], scores, masked_score)
        new_max = jnp.maximum(running_max, jnp.max(scores, axis=-1))
        rescale = jnp.exp(running_max - new_max)
        weights = jnp.where(allowed[None], jnp.exp(scores - new_max[..., None]), 0.0)
        new_sum = running_sum * rescale + jnp.sum(weights, axis=-1)
        added = jnp.einsum(
            "hqk,khe->hqe",
            weights.astype(jnp.bfloat16),
            value_rows,
            preferred_element_type=jnp.float32,
        )
        return (new_max, new_sum, accum * rescale[..., None] + added)

    def absorb(group_state, group, kblock, kstart):
        query_a, query_b, positions, last_pos = group
        block_rows = kblock.shape[0]
        k_pos = kstart + jnp.arange(block_rows, dtype=jnp.int32)
        allowed = k_pos[None, :] <= positions[:, None]
        keys_a = kblock[:, :width_q].reshape(block_rows, heads_dev, head_qk)
        keys_b = kblock[:, width_q : 2 * width_q].reshape(block_rows, heads_dev, head_qk)
        value_rows = kblock[:, 2 * width_q :].reshape(block_rows, heads_dev, head_v)
        first_map = one_map(query_a, keys_a, value_rows, allowed, *group_state[:3])
        second_map = one_map(query_b, keys_b, value_rows, allowed, *group_state[3:])
        return first_map + second_map

    group = groups[0]
    group_rows = group[0].shape[0]
    start_max = jnp.full((heads_dev, group_rows), masked_score, jnp.float32)
    start_sum = jnp.zeros((heads_dev, group_rows), jnp.float32)
    start_acc = jnp.zeros((heads_dev, group_rows, head_v), jnp.float32)
    initial_list = [(start_max, start_sum, start_acc, start_max, start_sum, start_acc)]
    initial = tuple(initial_list)
    softmax_state = initial
    kv_piece = lax.all_gather(key_values, "sp", axis=0, tiled=True)
    piece_rows = kv_piece.shape[0]
    block_rows = math.gcd(piece_rows, 512)
    block_count = piece_rows // block_rows
    stacked = kv_piece.reshape(block_count, block_rows, kv_piece.shape[1])

    def absorb_step(carried, blocks_in):
        kblock, block_index = blocks_in
        kstart = block_index * block_rows
        renewed = []
        for group, group_state in zip(groups, carried):
            renewed.append(
                lax.cond(
                    kstart <= group[3],
                    lambda inner, group=group: absorb(inner, group, kblock, kstart),
                    lambda inner: inner,
                    group_state,
                )
            )
        return (tuple(renewed), None)

    softmax_state, _ = lax.scan(
        absorb_step, softmax_state, (stacked, jnp.arange(block_count, dtype=jnp.int32))
    )
    normed_sets = []
    for group_state in softmax_state:
        out_a = group_state[2] / group_state[1][..., None]
        out_b = group_state[5] / group_state[4][..., None]
        mixed_out = out_a - lambdas[:, None, None] * out_b
        scale_rows = lax.rsqrt(jnp.mean(mixed_out * mixed_out, axis=-1, keepdims=True) + epsilon)
        normed = (mixed_out * scale_rows * norm_gain).astype(jnp.bfloat16)
        group_rows = normed.shape[1]
        normed_sets.append(jnp.transpose(normed, (1, 0, 2)).reshape(group_rows, heads_dev * head_v))
    normed_all = normed_sets[0]
    partial_value = jnp.dot(normed_all, out_proj, preferred_element_type=jnp.float32)
    result = lax.psum(partial_value.astype(jnp.bfloat16), "tp")
    return result


MESH = pl.DeviceIdType.MESH
PLANE = 4


def fused_kernel(
    groups,
    score_scale,
    hidden_hbm,
    q1_hbm,
    q2_hbm,
    k1_hbm,
    k2_hbm,
    v_hbm,
    lam_ref,
    gain_ref,
    wo_hbm,
    out_ref,
    hid,
    wq1,
    wq2,
    wk1,
    wk2,
    wv,
    wo,
    kv_out,
    q_out,
    kv_all,
    q_all,
    n_out,
    n_all,
    max_all,
    sum_all,
    acc_all,
    load_sem,
    wo_send,
    wo_recv,
    kv_send,
    kv_recv,
    q_send,
    q_recv,
    x_send,
    x_recv,
    y_send,
    y_recv,
    f_send,
    f_recv,
    n_send,
    n_recv,
    r_send,
    r_recv,
):
    me = lax.axis_index("sp")
    core = lax.axis_index("tp")
    plane = me // PLANE
    spot = lax.rem(me, PLANE)
    x_spot = spot + 1 - 2 * lax.rem(spot, 2)
    y_spot = spot + 2 - 4 * (spot // 2)
    rows = hid.shape[0]
    qk = q1_hbm.shape[1] // groups
    width = 2 * qk

    def load(index, src, dst):
        return pltpu.make_async_copy(src, dst, load_sem.at[index])

    loads = [
        load(0, hidden_hbm, hid),
        load(1, k1_hbm, wk1),
        load(2, k2_hbm, wk2),
        load(3, v_hbm, wv),
        load(4, q1_hbm, wq1),
        load(5, q2_hbm, wq2),
        load(6, wo_hbm, wo.at[core]),
    ]
    barrier = pltpu.get_barrier_semaphore()

    def greet(index, tp_index):
        pl.semaphore_signal(
            barrier, inc=1, device_id=(index, tp_index), device_id_type=MESH
        )

    for step in range(1, groups):
        other = lax.rem(plane + step, groups) * PLANE + spot
        greet(other, core)
    greet(me, 1 - core)
    greet(plane * PLANE + x_spot, core)
    greet(plane * PLANE + y_spot, core)

    for item in loads:
        item.start()

    def send(src, dst, send_sem, recv_sem, index, tp_index):
        return pltpu.make_async_remote_copy(
            src_ref=src,
            dst_ref=dst,
            send_sem=send_sem,
            recv_sem=recv_sem,
            device_id=(index, tp_index),
            device_id_type=MESH,
        )

    loads[0].wait()
    pending = []

    def project(weight_ref):
        return jnp.dot(hid[...], weight_ref[...], preferred_element_type=jnp.float32)

    loads[1].wait()
    first = project(wk1).astype(jnp.bfloat16)
    loads[2].wait()
    second = project(wk2).astype(jnp.bfloat16)
    for head in range(groups):
        cut = slice(head * qk, (head + 1) * qk)
        kv_out[head, :, :width] = jnp.concatenate((first[:, cut], second[:, cut]), axis=1)
    loads[3].wait()
    head_v = v_hbm.shape[1] // groups
    for head in range(groups):
        cut = slice(head * head_v, (head + 1) * head_v)
        kv_out[head, :, width:] = jnp.dot(
            hid[...], wv[:, cut], preferred_element_type=jnp.float32
        ).astype(jnp.bfloat16)
    kv_all[me] = kv_out[plane]
    pl.semaphore_wait(barrier, groups - 1 + 3)
    kv_copies = [None]
    for step in range(1, groups):
        target = lax.rem(plane + step, groups)
        copy = send(
            kv_out.at[target],
            kv_all.at[me],
            kv_send.at[step],
            kv_recv.at[step],
            target * PLANE + spot,
            core,
        )
        copy.start()
        kv_copies.append(copy)

    def from_plane(step):
        return lax.rem(plane - step + groups, groups)

    def spread(step):
        block = from_plane(step) * PLANE + spot
        for sems, where in (((x_send, x_recv), x_spot), ((y_send, y_recv), y_spot)):
            copy = send(
                kv_all.at[block],
                kv_all.at[block],
                sems[0].at[step],
                sems[1].at[step],
                plane * PLANE + where,
                core,
            )
            copy.start()
            pending.append(copy)

    def arrived(recv_sem, block):
        pltpu.make_async_copy(kv_all.at[block], kv_all.at[block], recv_sem).wait()

    def relay(step):
        x_block = from_plane(step) * PLANE + x_spot
        y_block = from_plane(step) * PLANE + y_spot
        arrived(x_recv.at[step], x_block)
        arrived(y_recv.at[step], y_block)
        block, where = (x_block, y_spot) if step % 2 == 0 else (y_block, x_spot)
        copy = send(
            kv_all.at[block],
            kv_all.at[block],
            f_send.at[step],
            f_recv.at[step],
            plane * PLANE + where,
            core,
        )
        copy.start()
        pending.append(copy)

    spread(0)

    loads[4].wait()
    first = (project(wq1) * score_scale).astype(jnp.bfloat16)
    loads[5].wait()
    second = (project(wq2) * score_scale).astype(jnp.bfloat16)
    for head in range(groups):
        cut = slice(head * qk, (head + 1) * qk)
        q_out[head] = jnp.concatenate((first[:, cut], second[:, cut]), axis=1)
    q_all[plane] = q_out[plane]
    q_copies = [None]
    for step in range(1, groups):
        target = lax.rem(plane + step, groups)
        copy = send(
            q_out.at[target],
            q_all.at[plane],
            q_send.at[step],
            q_recv.at[step],
            target * PLANE + spot,
            core,
        )
        copy.start()
        q_copies.append(copy)
    loads[6].wait()
    wo_copy = send(wo.at[core], wo.at[core], wo_send, wo_recv, me, 1 - core)
    wo_copy.start()

    def forward_arrival(step):
        arrived(kv_recv.at[step], from_plane(step) * PLANE + spot)
        spread(step)

    def stage_ready(step):
        arrived(f_recv.at[step], from_plane(step) * PLANE + (PLANE - 1 - spot))
        if step > 0:
            slot = q_all.at[from_plane(step)]
            pltpu.make_async_copy(slot, slot, q_recv.at[step]).wait()

    tile = ROW_TILE
    tiles = rows // tile
    chunk = PLANE * rows
    lane = lax.broadcasted_iota(jnp.int32, (tile, width), 1)
    lam = lam_ref[plane]
    gain = gain_ref[...]

    def pair_tile(group, key_group, part, diagonal):
        begin = pl.multiple_of(part * tile, tile)
        queries = q_all[group, pl.ds(begin, tile), :]
        zero = jnp.zeros_like(queries)
        both = jnp.concatenate(
            (jnp.where(lane < qk, queries, zero), jnp.where(lane >= qk, queries, zero)), axis=0
        )
        block = kv_all[pl.ds(key_group * PLANE, PLANE)].reshape(chunk, width + head_v)
        scores = lax.dot_general(
            both,
            block[:, :width],
            (((1,), (1,)), ((), ())),
            preferred_element_type=jnp.float32,
        )
        if diagonal:
            q_pos = spot * rows + begin + lax.rem(
                lax.broadcasted_iota(jnp.int32, (2 * tile, chunk), 0), tile
            )
            k_pos = lax.broadcasted_iota(jnp.int32, (2 * tile, chunk), 1)
            scores = jnp.where(k_pos <= q_pos, scores, masked_score)
        new_max = jnp.max(scores, axis=-1, keepdims=True)
        if not diagonal:
            running_max = max_all[group, part]
            new_max = jnp.maximum(running_max, new_max)
            rescale = jnp.exp2(running_max - new_max)
        weights = jnp.exp2(scores - new_max)
        new_sum = jnp.sum(weights, axis=-1, keepdims=True)
        accum = jnp.dot(
            weights.astype(jnp.bfloat16),
            block[:, width:],
            preferred_element_type=jnp.float32,
        )
        if not diagonal:
            new_sum = sum_all[group, part] * rescale + new_sum
            accum = acc_all[group, part] * rescale + accum
        max_all[group, part] = new_max
        sum_all[group, part] = new_sum
        acc_all[group, part] = accum

    def pair(group, key_group, diagonal):
        lax.fori_loop(
            0, tiles, lambda t, c: (pair_tile(group, key_group, t, diagonal), c)[1], 0
        )

    def meet(step, earlier):
        one, other = from_plane(step), from_plane(earlier)
        pair(jnp.maximum(one, other), jnp.minimum(one, other), False)

    def normed_copy(group):
        return send(
            n_out.at[group],
            n_all.at[core, plane],
            n_send.at[group],
            n_recv.at[plane],
            group * PLANE + spot,
            core,
        )

    def partner_copy(head):
        slot = n_all.at[core, head]
        return send(slot, slot, r_send.at[head], r_recv.at[head], me, 1 - core)

    def finish(group):
        def finish_tile(part, _):
            begin = pl.multiple_of(part * tile, tile)
            heads_out = acc_all[group, part] / sum_all[group, part]
            mixed = heads_out[:tile] - lam * heads_out[tile:]
            scale_rows = lax.rsqrt(jnp.mean(mixed * mixed, axis=-1, keepdims=True) + epsilon)
            normed = (mixed * scale_rows * gain).astype(jnp.bfloat16)
            n_out[group, pl.ds(begin, tile), :] = normed
            return 0

        lax.fori_loop(0, tiles, finish_tile, 0)

    forward_arrival(1)
    relay(0)
    stage_ready(0)
    pair(plane, plane, True)
    for step in range(1, groups):
        if step + 1 < groups:
            forward_arrival(step + 1)
        relay(step)
        stage_ready(step)
        pair(from_plane(step), from_plane(step), True)
        if step + 1 < groups:
            for earlier in range(step):
                meet(step, earlier)
        else:
            for earlier in list(range(1, step)) + [0]:
                meet(step, earlier)
                finish(from_plane(earlier))
                if earlier == 0:
                    n_all[core, plane] = n_out[plane]
                    partner_copy(plane).start()
                else:
                    normed_copy(from_plane(earlier)).start()
    finish(from_plane(groups - 1))
    normed_copy(from_plane(groups - 1)).start()

    for step in range(1, groups):
        head = from_plane(step)
        slot = n_all.at[core, head]
        pltpu.make_async_copy(slot, slot, n_recv.at[head]).wait()
        partner_copy(head).start()
    wo_copy.wait_send()

    def out_tiles(tp_index, first_part):
        normed = jnp.concatenate([n_all[tp_index, head] for head in range(groups)], axis=1)

        def out_tile(index, _):
            columns = pl.ds(pl.multiple_of(index * OUT_TILE, OUT_TILE), OUT_TILE)
            part = jnp.dot(normed, wo[tp_index, :, columns], preferred_element_type=jnp.float32)
            part = part.astype(jnp.bfloat16)
            if not first_part:
                part = (part.astype(jnp.float32) + out_ref[:, columns].astype(jnp.float32)).astype(
                    jnp.bfloat16
                )
            out_ref[:, columns] = part
            return 0

        lax.fori_loop(0, out_ref.shape[1] // OUT_TILE, out_tile, 0)

    out_tiles(core, True)
    pltpu.make_async_copy(wo.at[1 - core], wo.at[1 - core], wo_recv).wait()
    for head in range(groups):
        slot = n_all.at[1 - core, head]
        pltpu.make_async_copy(slot, slot, r_recv.at[head]).wait()
    out_tiles(1 - core, False)

    for copy in pending:
        copy.wait_send()
    for step in range(1, groups):
        kv_copies[step].wait_send()
        q_copies[step].wait_send()
        normed_copy(from_plane(step)).wait_send()
    for head in range(groups):
        partner_copy(head).wait_send()


ROW_TILE = 128
OUT_TILE = 256


def fused_shards(
    hidden_in, query_one, query_two, key_one, key_two, value_proj, lambdas, norm_gain, out_proj
):
    groups = lambdas.shape[0]
    rows, depth = hidden_in.shape
    head_qk = query_one.shape[1] // groups
    head_v = value_proj.shape[1] // groups
    width = 2 * head_qk
    blocks = groups * PLANE
    columns = out_proj.shape[1]
    score_scale = 1.75 * head_qk ** (-0.5) * math.log2(math.e)
    bf16 = jnp.bfloat16
    dma = pltpu.SemaphoreType.DMA
    hbm = pl.BlockSpec(memory_space=pl.ANY)
    vmem = pl.BlockSpec(memory_space=pltpu.VMEM)
    smem = pl.BlockSpec(memory_space=pltpu.SMEM)

    def body(*refs):
        fused_kernel(groups, score_scale, *refs)

    return pl.pallas_call(
        body,
        name="fused_attention",
        out_shape=jax.ShapeDtypeStruct((rows, columns), bf16),
        in_specs=[hbm] * 6 + [smem, vmem, hbm],
        out_specs=vmem,
        scratch_shapes=[
            pltpu.VMEM(hidden_in.shape, bf16),
            pltpu.VMEM(query_one.shape, bf16),
            pltpu.VMEM(query_two.shape, bf16),
            pltpu.VMEM(key_one.shape, bf16),
            pltpu.VMEM(key_two.shape, bf16),
            pltpu.VMEM(value_proj.shape, bf16),
            pltpu.VMEM((2,) + out_proj.shape, bf16),
            pltpu.VMEM((groups, rows, width + head_v), bf16),
            pltpu.VMEM((groups, rows, width), bf16),
            pltpu.VMEM((blocks, rows, width + head_v), bf16),
            pltpu.VMEM((groups, rows, width), bf16),
            pltpu.VMEM((groups, rows, head_v), bf16),
            pltpu.VMEM((2, groups, rows, head_v), bf16),
            pltpu.VMEM((groups, rows // ROW_TILE, 2 * ROW_TILE, 1), jnp.float32),
            pltpu.VMEM((groups, rows // ROW_TILE, 2 * ROW_TILE, 1), jnp.float32),
            pltpu.VMEM((groups, rows // ROW_TILE, 2 * ROW_TILE, head_v), jnp.float32),
            dma((7,)),
            dma,
            dma,
        ]
        + [dma((groups,))] * 14,
        compiler_params=pltpu.CompilerParams(
            collective_id=0, has_side_effects=True, vmem_limit_bytes=60 * 1024 * 1024
        ),
    )(
        hidden_in,
        query_one,
        query_two,
        key_one,
        key_two,
        value_proj,
        lambdas,
        norm_gain.reshape(1, head_v),
        out_proj,
    )


def solution(mesh):
    placed = (
        P("sp", None),
        P(None, "tp"),
        P(None, "tp"),
        P(None, "tp"),
        P(None, "tp"),
        P(None, "tp"),
        P("tp"),
        P(),
        P("tp", None),
    )

    def body(*args):
        groups = args[6].shape[0]
        split = groups * PLANE == mesh.shape["sp"] and mesh.shape["tp"] == 2
        return (fused_shards if split else shards)(*args)

    return jax.shard_map(
        body, mesh=mesh, in_specs=placed, out_specs=P("sp", None), check_vma=False
    )
```

```python
import math

import jax
import jax.numpy as jnp
from jax import lax
from jax.experimental import pallas as pl
from jax.experimental.pallas import tpu as pltpu
from jax.sharding import PartitionSpec as P

epsilon = 1e-06
masked_score = -1e30


def shards(
    hidden_in, query_one, query_two, key_one, key_two, value_proj, lambdas, norm_gain, out_proj
):
    heads_dev = lambdas.shape[0]
    head_qk = query_one.shape[1] // heads_dev
    head_v = value_proj.shape[1] // heads_dev
    width_q = heads_dev * head_qk
    score_scale = 1.75 * head_qk ** (-0.5)
    joined = jnp.concatenate((query_one, query_two, key_one, key_two, value_proj), axis=1)
    projected = jnp.dot(hidden_in, joined, preferred_element_type=jnp.float32).astype(jnp.bfloat16)
    tok_rows = projected.shape[0]
    key_values = projected[:, 2 * width_q :]
    my_index = lax.axis_index("sp")
    offset = my_index * tok_rows
    query_sets = (projected[:, : 2 * width_q],)
    position_sets = (offset + jnp.arange(tok_rows, dtype=jnp.int32),)
    groups = []
    for query_rows, positions in zip(query_sets, position_sets):
        group_rows = query_rows.shape[0]
        query_a = query_rows[:, :width_q].reshape(group_rows, heads_dev, head_qk)
        query_b = query_rows[:, width_q:].reshape(group_rows, heads_dev, head_qk)
        groups.append((query_a, query_b, positions, positions[group_rows - 1]))

    def one_map(queries, keys, value_rows, allowed, running_max, running_sum, accum):
        scores = (
            jnp.einsum("qhd,khd->hqk", queries, keys, preferred_element_type=jnp.float32)
            * score_scale
        )
        scores = jnp.where(allowed[None], scores, masked_score)
        new_max = jnp.maximum(running_max, jnp.max(scores, axis=-1))
        rescale = jnp.exp(running_max - new_max)
        weights = jnp.where(allowed[None], jnp.exp(scores - new_max[..., None]), 0.0)
        new_sum = running_sum * rescale + jnp.sum(weights, axis=-1)
        added = jnp.einsum(
            "hqk,khe->hqe",
            weights.astype(jnp.bfloat16),
            value_rows,
            preferred_element_type=jnp.float32,
        )
        return (new_max, new_sum, accum * rescale[..., None] + added)

    def absorb(group_state, group, kblock, kstart):
        query_a, query_b, positions, last_pos = group
        block_rows = kblock.shape[0]
        k_pos = kstart + jnp.arange(block_rows, dtype=jnp.int32)
        allowed = k_pos[None, :] <= positions[:, None]
        keys_a = kblock[:, :width_q].reshape(block_rows, heads_dev, head_qk)
        keys_b = kblock[:, width_q : 2 * width_q].reshape(block_rows, heads_dev, head_qk)
        value_rows = kblock[:, 2 * width_q :].reshape(block_rows, heads_dev, head_v)
        first_map = one_map(query_a, keys_a, value_rows, allowed, *group_state[:3])
        second_map = one_map(query_b, keys_b, value_rows, allowed, *group_state[3:])
        return first_map + second_map

    group = groups[0]
    group_rows = group[0].shape[0]
    start_max = jnp.full((heads_dev, group_rows), masked_score, jnp.float32)
    start_sum = jnp.zeros((heads_dev, group_rows), jnp.float32)
    start_acc = jnp.zeros((heads_dev, group_rows, head_v), jnp.float32)
    initial_list = [(start_max, start_sum, start_acc, start_max, start_sum, start_acc)]
    initial = tuple(initial_list)
    softmax_state = initial
    kv_piece = lax.all_gather(key_values, "sp", axis=0, tiled=True)
    piece_rows = kv_piece.shape[0]
    block_rows = math.gcd(piece_rows, 512)
    block_count = piece_rows // block_rows
    stacked = kv_piece.reshape(block_count, block_rows, kv_piece.shape[1])

    def absorb_step(carried, blocks_in):
        kblock, block_index = blocks_in
        kstart = block_index * block_rows
        renewed = []
        for group, group_state in zip(groups, carried):
            renewed.append(
                lax.cond(
                    kstart <= group[3],
                    lambda inner, group=group: absorb(inner, group, kblock, kstart),
                    lambda inner: inner,
                    group_state,
                )
            )
        return (tuple(renewed), None)

    softmax_state, _ = lax.scan(
        absorb_step, softmax_state, (stacked, jnp.arange(block_count, dtype=jnp.int32))
    )
    normed_sets = []
    for group_state in softmax_state:
        out_a = group_state[2] / group_state[1][..., None]
        out_b = group_state[5] / group_state[4][..., None]
        mixed_out = out_a - lambdas[:, None, None] * out_b
        scale_rows = lax.rsqrt(jnp.mean(mixed_out * mixed_out, axis=-1, keepdims=True) + epsilon)
        normed = (mixed_out * scale_rows * norm_gain).astype(jnp.bfloat16)
        group_rows = normed.shape[1]
        normed_sets.append(jnp.transpose(normed, (1, 0, 2)).reshape(group_rows, heads_dev * head_v))
    normed_all = normed_sets[0]
    partial_value = jnp.dot(normed_all, out_proj, preferred_element_type=jnp.float32)
    result = lax.psum(partial_value.astype(jnp.bfloat16), "tp")
    return result


MESH = pl.DeviceIdType.MESH
PLANE = 4


def fused_kernel(
    groups,
    score_scale,
    hidden_hbm,
    q1_hbm,
    q2_hbm,
    k1_hbm,
    k2_hbm,
    v_hbm,
    lam_ref,
    gain_ref,
    wo_hbm,
    out_ref,
    hid,
    wq1,
    wq2,
    wk1,
    wk2,
    wv,
    wo,
    kv_out,
    q_out,
    kv_all,
    q_all,
    n_out,
    n_all,
    max_all,
    sum_all,
    acc_all,
    load_sem,
    wo_send,
    wo_recv,
    kv_send,
    kv_recv,
    q_send,
    q_recv,
    x_send,
    x_recv,
    y_send,
    y_recv,
    f_send,
    f_recv,
    n_send,
    n_recv,
    r_send,
    r_recv,
):
    me = lax.axis_index("sp")
    core = lax.axis_index("tp")
    plane = me // PLANE
    spot = lax.rem(me, PLANE)
    x_spot = spot + 1 - 2 * lax.rem(spot, 2)
    y_spot = spot + 2 - 4 * (spot // 2)
    rows = hid.shape[0]
    qk = q1_hbm.shape[1] // groups
    width = 2 * qk

    def load(index, src, dst):
        return pltpu.make_async_copy(src, dst, load_sem.at[index])

    loads = [
        load(0, hidden_hbm, hid),
        load(1, k1_hbm, wk1),
        load(2, k2_hbm, wk2),
        load(3, v_hbm, wv),
        load(4, q1_hbm, wq1),
        load(5, q2_hbm, wq2),
        load(6, wo_hbm, wo.at[core]),
    ]
    barrier = pltpu.get_barrier_semaphore()

    def greet(index, tp_index):
        pl.semaphore_signal(
            barrier, inc=1, device_id=(index, tp_index), device_id_type=MESH
        )

    for step in range(1, groups):
        other = lax.rem(plane + step, groups) * PLANE + spot
        greet(other, core)
    greet(me, 1 - core)
    greet(plane * PLANE + x_spot, core)
    greet(plane * PLANE + y_spot, core)

    for item in loads:
        item.start()

    def send(src, dst, send_sem, recv_sem, index, tp_index):
        return pltpu.make_async_remote_copy(
            src_ref=src,
            dst_ref=dst,
            send_sem=send_sem,
            recv_sem=recv_sem,
            device_id=(index, tp_index),
            device_id_type=MESH,
        )

    upper = plane >= groups // 2
    mirrored = jnp.where(upper, groups - 1 - plane, plane)

    def from_plane(step):
        if step == 0:
            return plane
        near = jnp.where(step - 1 < mirrored, step - 1, step)
        return jnp.where(upper, groups - 1 - near, near)

    loads[0].wait()
    pending = []

    def project(weight_ref):
        return jnp.dot(hid[...], weight_ref[...], preferred_element_type=jnp.float32)

    loads[1].wait()
    first = project(wk1).astype(jnp.bfloat16)
    loads[2].wait()
    second = project(wk2).astype(jnp.bfloat16)
    for head in range(groups):
        cut = slice(head * qk, (head + 1) * qk)
        kv_out[head, :, :width] = jnp.concatenate((first[:, cut], second[:, cut]), axis=1)
    loads[3].wait()
    head_v = v_hbm.shape[1] // groups
    for head in range(groups):
        cut = slice(head * head_v, (head + 1) * head_v)
        kv_out[head, :, width:] = jnp.dot(
            hid[...], wv[:, cut], preferred_element_type=jnp.float32
        ).astype(jnp.bfloat16)
    kv_all[me] = kv_out[plane]
    loads[4].wait()
    first = (project(wq1) * score_scale).astype(jnp.bfloat16)
    loads[5].wait()
    second = (project(wq2) * score_scale).astype(jnp.bfloat16)
    for head in range(groups):
        cut = slice(head * qk, (head + 1) * qk)
        q_out[head] = jnp.concatenate((first[:, cut], second[:, cut]), axis=1)
    q_all[plane] = q_out[plane]
    pl.semaphore_wait(barrier, groups - 1 + 3)

    def kv_copy(step):
        target = from_plane(step)
        return send(
            kv_out.at[target],
            kv_all.at[me],
            kv_send.at[step],
            kv_recv.at[plane],
            target * PLANE + spot,
            core,
        )

    def q_copy(step):
        target = from_plane(step)
        return send(
            q_out.at[target],
            q_all.at[plane],
            q_send.at[step],
            q_recv.at[plane],
            target * PLANE + spot,
            core,
        )

    def spread(step):
        block = from_plane(step) * PLANE + spot
        for sems, where in (((x_send, x_recv), x_spot), ((y_send, y_recv), y_spot)):
            copy = send(
                kv_all.at[block],
                kv_all.at[block],
                sems[0].at[step],
                sems[1].at[step],
                plane * PLANE + where,
                core,
            )
            copy.start()
            pending.append(copy)

    def arrived(recv_sem, block):
        pltpu.make_async_copy(kv_all.at[block], kv_all.at[block], recv_sem).wait()

    half = rows // 2

    def relay(step):
        x_block = from_plane(step) * PLANE + x_spot
        y_block = from_plane(step) * PLANE + y_spot
        for part, block, sem, where in (
            (0, x_block, x_recv, y_spot),
            (1, y_block, y_recv, x_spot),
        ):
            arrived(sem.at[step], block)
            piece = kv_all.at[block, pl.ds(part * half, half), :]
            copy = send(
                piece,
                piece,
                f_send.at[step, part],
                f_recv.at[step, part],
                plane * PLANE + where,
                core,
            )
            copy.start()
            pending.append(copy)

    kv_copy(1).start()
    spread(0)
    for step in range(2, groups):
        kv_copy(step).start()
        q_copy(step - 1).start()
    q_copy(groups - 1).start()
    loads[6].wait()
    wo_copy = send(wo.at[core], wo.at[core], wo_send, wo_recv, me, 1 - core)
    wo_copy.start()

    def forward_arrival(step):
        arrived(kv_recv.at[from_plane(step)], from_plane(step) * PLANE + spot)
        spread(step)

    def stage_ready(step):
        far = from_plane(step) * PLANE + (PLANE - 1 - spot)
        for part in range(2):
            piece = kv_all.at[far, pl.ds(part * half, half), :]
            pltpu.make_async_copy(piece, piece, f_recv.at[step, part]).wait()
        if step > 0:
            slot = q_all.at[from_plane(step)]
            pltpu.make_async_copy(slot, slot, q_recv.at[from_plane(step)]).wait()

    tile = ROW_TILE
    tiles = rows // tile
    chunk = PLANE * rows
    lane = lax.broadcasted_iota(jnp.int32, (tile, width), 1)
    lam = lam_ref[plane]
    gain = gain_ref[...]

    def pair_tile(group, key_group, part, diagonal):
        begin = pl.multiple_of(part * tile, tile)
        queries = q_all[group, pl.ds(begin, tile), :]
        zero = jnp.zeros_like(queries)
        both = jnp.concatenate(
            (jnp.where(lane < qk, queries, zero), jnp.where(lane >= qk, queries, zero)), axis=0
        )
        block = kv_all[pl.ds(key_group * PLANE, PLANE)].reshape(chunk, width + head_v)
        scores = lax.dot_general(
            both,
            block[:, :width],
            (((1,), (1,)), ((), ())),
            preferred_element_type=jnp.float32,
        )
        if diagonal:
            q_pos = spot * rows + begin + lax.rem(
                lax.broadcasted_iota(jnp.int32, (2 * tile, chunk), 0), tile
            )
            k_pos = lax.broadcasted_iota(jnp.int32, (2 * tile, chunk), 1)
            scores = jnp.where(k_pos <= q_pos, scores, masked_score)
        new_max = jnp.max(scores, axis=-1, keepdims=True)
        if not diagonal:
            running_max = max_all[group, part]
            new_max = jnp.maximum(running_max, new_max)
            rescale = jnp.exp2(running_max - new_max)
        weights = jnp.exp2(scores - new_max)
        new_sum = jnp.sum(weights, axis=-1, keepdims=True)
        accum = jnp.dot(
            weights.astype(jnp.bfloat16),
            block[:, width:],
            preferred_element_type=jnp.float32,
        )
        if not diagonal:
            new_sum = sum_all[group, part] * rescale + new_sum
            accum = acc_all[group, part] * rescale + accum
        max_all[group, part] = new_max
        sum_all[group, part] = new_sum
        acc_all[group, part] = accum

    def pair(group, key_group, diagonal):
        lax.fori_loop(
            0, tiles, lambda t, c: (pair_tile(group, key_group, t, diagonal), c)[1], 0
        )

    def meet(step, earlier):
        one, other = from_plane(step), from_plane(earlier)
        pair(jnp.maximum(one, other), jnp.minimum(one, other), False)

    def normed_copy(group):
        return send(
            n_out.at[group],
            n_all.at[core, plane],
            n_send.at[group],
            n_recv.at[plane],
            group * PLANE + spot,
            core,
        )

    def partner_copy(head):
        slot = n_all.at[core, head]
        return send(slot, slot, r_send.at[head], r_recv.at[head], me, 1 - core)

    def finish(group):
        def finish_tile(part, _):
            begin = pl.multiple_of(part * tile, tile)
            heads_out = acc_all[group, part] / sum_all[group, part]
            mixed = heads_out[:tile] - lam * heads_out[tile:]
            scale_rows = lax.rsqrt(jnp.mean(mixed * mixed, axis=-1, keepdims=True) + epsilon)
            normed = (mixed * scale_rows * gain).astype(jnp.bfloat16)
            n_out[group, pl.ds(begin, tile), :] = normed
            return 0

        lax.fori_loop(0, tiles, finish_tile, 0)

    def stage(step):
        stage_ready(step)
        pair(from_plane(step), from_plane(step), True)
        if step + 1 < groups:
            for earlier in range(step):
                meet(step, earlier)
        else:
            for earlier in list(range(1, step)) + [0]:
                meet(step, earlier)
                finish(from_plane(earlier))
                if earlier == 0:
                    n_all[core, plane] = n_out[plane]
                    partner_copy(plane).start()
                else:
                    normed_copy(from_plane(earlier)).start()

    for step in range(1, groups):
        forward_arrival(step)
        relay(step - 1)
        if step >= 2:
            stage(step - 2)
    relay(groups - 1)
    stage(groups - 2)
    stage(groups - 1)
    finish(from_plane(groups - 1))
    normed_copy(from_plane(groups - 1)).start()

    for step in range(1, groups):
        head = from_plane(step)
        slot = n_all.at[core, head]
        pltpu.make_async_copy(slot, slot, n_recv.at[head]).wait()
        partner_copy(head).start()
    wo_copy.wait_send()

    def out_tiles(tp_index, first_part):
        normed = jnp.concatenate([n_all[tp_index, head] for head in range(groups)], axis=1)

        def out_tile(index, _):
            columns = pl.ds(pl.multiple_of(index * OUT_TILE, OUT_TILE), OUT_TILE)
            part = jnp.dot(normed, wo[tp_index, :, columns], preferred_element_type=jnp.float32)
            part = part.astype(jnp.bfloat16)
            if not first_part:
                part = (part.astype(jnp.float32) + out_ref[:, columns].astype(jnp.float32)).astype(
                    jnp.bfloat16
                )
            out_ref[:, columns] = part
            return 0

        lax.fori_loop(0, out_ref.shape[1] // OUT_TILE, out_tile, 0)

    out_tiles(core, True)
    pltpu.make_async_copy(wo.at[1 - core], wo.at[1 - core], wo_recv).wait()
    for head in range(groups):
        slot = n_all.at[1 - core, head]
        pltpu.make_async_copy(slot, slot, r_recv.at[head]).wait()
    out_tiles(1 - core, False)

    for copy in pending:
        copy.wait_send()
    for step in range(1, groups):
        kv_copy(step).wait_send()
        q_copy(step).wait_send()
        normed_copy(from_plane(step)).wait_send()
    for head in range(groups):
        partner_copy(head).wait_send()


ROW_TILE = 256
OUT_TILE = 256


def fused_shards(
    hidden_in, query_one, query_two, key_one, key_two, value_proj, lambdas, norm_gain, out_proj
):
    groups = lambdas.shape[0]
    rows, depth = hidden_in.shape
    head_qk = query_one.shape[1] // groups
    head_v = value_proj.shape[1] // groups
    width = 2 * head_qk
    blocks = groups * PLANE
    columns = out_proj.shape[1]
    score_scale = 1.75 * head_qk ** (-0.5) * math.log2(math.e)
    bf16 = jnp.bfloat16
    dma = pltpu.SemaphoreType.DMA
    hbm = pl.BlockSpec(memory_space=pl.ANY)
    vmem = pl.BlockSpec(memory_space=pltpu.VMEM)
    smem = pl.BlockSpec(memory_space=pltpu.SMEM)

    def body(*refs):
        fused_kernel(groups, score_scale, *refs)

    return pl.pallas_call(
        body,
        name="fused_attention",
        out_shape=jax.ShapeDtypeStruct((rows, columns), bf16),
        in_specs=[hbm] * 6 + [smem, vmem, hbm],
        out_specs=vmem,
        scratch_shapes=[
            pltpu.VMEM(hidden_in.shape, bf16),
            pltpu.VMEM(query_one.shape, bf16),
            pltpu.VMEM(query_two.shape, bf16),
            pltpu.VMEM(key_one.shape, bf16),
            pltpu.VMEM(key_two.shape, bf16),
            pltpu.VMEM(value_proj.shape, bf16),
            pltpu.VMEM((2,) + out_proj.shape, bf16),
            pltpu.VMEM((groups, rows, width + head_v), bf16),
            pltpu.VMEM((groups, rows, width), bf16),
            pltpu.VMEM((blocks, rows, width + head_v), bf16),
            pltpu.VMEM((groups, rows, width), bf16),
            pltpu.VMEM((groups, rows, head_v), bf16),
            pltpu.VMEM((2, groups, rows, head_v), bf16),
            pltpu.VMEM((groups, rows // ROW_TILE, 2 * ROW_TILE, 1), jnp.float32),
            pltpu.VMEM((groups, rows // ROW_TILE, 2 * ROW_TILE, 1), jnp.float32),
            pltpu.VMEM((groups, rows // ROW_TILE, 2 * ROW_TILE, head_v), jnp.float32),
            dma((7,)),
            dma,
            dma,
        ]
        + [dma((groups,))] * 8
        + [dma((groups, 2))] * 2
        + [dma((groups,))] * 4,
        compiler_params=pltpu.CompilerParams(
            collective_id=0, has_side_effects=True, vmem_limit_bytes=60 * 1024 * 1024
        ),
    )(
        hidden_in,
        query_one,
        query_two,
        key_one,
        key_two,
        value_proj,
        lambdas,
        norm_gain.reshape(1, head_v),
        out_proj,
    )


def solution(mesh):
    placed = (
        P("sp", None),
        P(None, "tp"),
        P(None, "tp"),
        P(None, "tp"),
        P(None, "tp"),
        P(None, "tp"),
        P("tp"),
        P(),
        P("tp", None),
    )

    def body(*args):
        groups = args[6].shape[0]
        split = groups * PLANE == mesh.shape["sp"] and mesh.shape["tp"] == 2
        return (fused_shards if split else shards)(*args)

    return jax.shard_map(
        body, mesh=mesh, in_specs=placed, out_specs=P("sp", None), check_vma=False
    )
```

```python
import math

import jax
import jax.numpy as jnp
from jax import lax
from jax.experimental import pallas as pl
from jax.experimental.pallas import tpu as pltpu
from jax.sharding import PartitionSpec as P

epsilon = 1e-06
masked_score = -1e30


def shards(
    hidden_in, query_one, query_two, key_one, key_two, value_proj, lambdas, norm_gain, out_proj
):
    heads_dev = lambdas.shape[0]
    head_qk = query_one.shape[1] // heads_dev
    head_v = value_proj.shape[1] // heads_dev
    width_q = heads_dev * head_qk
    score_scale = 1.75 * head_qk ** (-0.5)
    joined = jnp.concatenate((query_one, query_two, key_one, key_two, value_proj), axis=1)
    projected = jnp.dot(hidden_in, joined, preferred_element_type=jnp.float32).astype(jnp.bfloat16)
    tok_rows = projected.shape[0]
    key_values = projected[:, 2 * width_q :]
    my_index = lax.axis_index("sp")
    offset = my_index * tok_rows
    query_sets = (projected[:, : 2 * width_q],)
    position_sets = (offset + jnp.arange(tok_rows, dtype=jnp.int32),)
    groups = []
    for query_rows, positions in zip(query_sets, position_sets):
        group_rows = query_rows.shape[0]
        query_a = query_rows[:, :width_q].reshape(group_rows, heads_dev, head_qk)
        query_b = query_rows[:, width_q:].reshape(group_rows, heads_dev, head_qk)
        groups.append((query_a, query_b, positions, positions[group_rows - 1]))

    def one_map(queries, keys, value_rows, allowed, running_max, running_sum, accum):
        scores = (
            jnp.einsum("qhd,khd->hqk", queries, keys, preferred_element_type=jnp.float32)
            * score_scale
        )
        scores = jnp.where(allowed[None], scores, masked_score)
        new_max = jnp.maximum(running_max, jnp.max(scores, axis=-1))
        rescale = jnp.exp(running_max - new_max)
        weights = jnp.where(allowed[None], jnp.exp(scores - new_max[..., None]), 0.0)
        new_sum = running_sum * rescale + jnp.sum(weights, axis=-1)
        added = jnp.einsum(
            "hqk,khe->hqe",
            weights.astype(jnp.bfloat16),
            value_rows,
            preferred_element_type=jnp.float32,
        )
        return (new_max, new_sum, accum * rescale[..., None] + added)

    def absorb(group_state, group, kblock, kstart):
        query_a, query_b, positions, last_pos = group
        block_rows = kblock.shape[0]
        k_pos = kstart + jnp.arange(block_rows, dtype=jnp.int32)
        allowed = k_pos[None, :] <= positions[:, None]
        keys_a = kblock[:, :width_q].reshape(block_rows, heads_dev, head_qk)
        keys_b = kblock[:, width_q : 2 * width_q].reshape(block_rows, heads_dev, head_qk)
        value_rows = kblock[:, 2 * width_q :].reshape(block_rows, heads_dev, head_v)
        first_map = one_map(query_a, keys_a, value_rows, allowed, *group_state[:3])
        second_map = one_map(query_b, keys_b, value_rows, allowed, *group_state[3:])
        return first_map + second_map

    group = groups[0]
    group_rows = group[0].shape[0]
    start_max = jnp.full((heads_dev, group_rows), masked_score, jnp.float32)
    start_sum = jnp.zeros((heads_dev, group_rows), jnp.float32)
    start_acc = jnp.zeros((heads_dev, group_rows, head_v), jnp.float32)
    initial_list = [(start_max, start_sum, start_acc, start_max, start_sum, start_acc)]
    initial = tuple(initial_list)
    softmax_state = initial
    kv_piece = lax.all_gather(key_values, "sp", axis=0, tiled=True)
    piece_rows = kv_piece.shape[0]
    block_rows = math.gcd(piece_rows, 512)
    block_count = piece_rows // block_rows
    stacked = kv_piece.reshape(block_count, block_rows, kv_piece.shape[1])

    def absorb_step(carried, blocks_in):
        kblock, block_index = blocks_in
        kstart = block_index * block_rows
        renewed = []
        for group, group_state in zip(groups, carried):
            renewed.append(
                lax.cond(
                    kstart <= group[3],
                    lambda inner, group=group: absorb(inner, group, kblock, kstart),
                    lambda inner: inner,
                    group_state,
                )
            )
        return (tuple(renewed), None)

    softmax_state, _ = lax.scan(
        absorb_step, softmax_state, (stacked, jnp.arange(block_count, dtype=jnp.int32))
    )
    normed_sets = []
    for group_state in softmax_state:
        out_a = group_state[2] / group_state[1][..., None]
        out_b = group_state[5] / group_state[4][..., None]
        mixed_out = out_a - lambdas[:, None, None] * out_b
        scale_rows = lax.rsqrt(jnp.mean(mixed_out * mixed_out, axis=-1, keepdims=True) + epsilon)
        normed = (mixed_out * scale_rows * norm_gain).astype(jnp.bfloat16)
        group_rows = normed.shape[1]
        normed_sets.append(jnp.transpose(normed, (1, 0, 2)).reshape(group_rows, heads_dev * head_v))
    normed_all = normed_sets[0]
    partial_value = jnp.dot(normed_all, out_proj, preferred_element_type=jnp.float32)
    result = lax.psum(partial_value.astype(jnp.bfloat16), "tp")
    return result


MESH = pl.DeviceIdType.MESH
PLANE = 4


def fused_kernel(
    groups,
    score_scale,
    hidden_hbm,
    q1_hbm,
    q2_hbm,
    k1_hbm,
    k2_hbm,
    v_hbm,
    lam_ref,
    gain_ref,
    wo_hbm,
    out_ref,
    hid,
    wq1,
    wq2,
    wk1,
    wk2,
    wv,
    wo,
    kv_out,
    q_out,
    kv_all,
    q_all,
    n_out,
    n_all,
    max_all,
    sum_all,
    acc_all,
    load_sem,
    wo_send,
    wo_recv,
    kv_send,
    kv_recv,
    q_send,
    q_recv,
    x_send,
    x_recv,
    y_send,
    y_recv,
    f_send,
    f_recv,
    n_send,
    n_recv,
    r_send,
    r_recv,
):
    me = lax.axis_index("sp")
    core = lax.axis_index("tp")
    plane = me // PLANE
    spot = lax.rem(me, PLANE)
    x_spot = spot + 1 - 2 * lax.rem(spot, 2)
    y_spot = spot + 2 - 4 * (spot // 2)
    rows = hid.shape[0]
    qk = q1_hbm.shape[1] // groups
    width = 2 * qk

    def load(index, src, dst):
        return pltpu.make_async_copy(src, dst, load_sem.at[index])

    loads = [
        load(0, hidden_hbm, hid),
        load(1, k1_hbm, wk1),
        load(2, k2_hbm, wk2),
        load(3, v_hbm, wv),
        load(4, q1_hbm, wq1),
        load(5, q2_hbm, wq2),
        load(6, wo_hbm, wo.at[core]),
    ]
    barrier = pltpu.get_barrier_semaphore()

    def greet(index, tp_index):
        pl.semaphore_signal(
            barrier, inc=1, device_id=(index, tp_index), device_id_type=MESH
        )

    for step in range(1, groups):
        other = lax.rem(plane + step, groups) * PLANE + spot
        greet(other, core)
    greet(me, 1 - core)
    greet(plane * PLANE + x_spot, core)
    greet(plane * PLANE + y_spot, core)

    for item in loads:
        item.start()

    def send(src, dst, send_sem, recv_sem, index, tp_index):
        return pltpu.make_async_remote_copy(
            src_ref=src,
            dst_ref=dst,
            send_sem=send_sem,
            recv_sem=recv_sem,
            device_id=(index, tp_index),
            device_id_type=MESH,
        )

    upper = plane >= groups // 2
    mirrored = jnp.where(upper, groups - 1 - plane, plane)

    def from_plane(step):
        if step == 0:
            return plane
        near = jnp.where(step - 1 < mirrored, step - 1, step)
        return jnp.where(upper, groups - 1 - near, near)

    loads[0].wait()
    pending = []

    def project(weight_ref):
        return jnp.dot(hid[...], weight_ref[...], preferred_element_type=jnp.float32)

    loads[1].wait()
    first = project(wk1).astype(jnp.bfloat16)
    loads[2].wait()
    second = project(wk2).astype(jnp.bfloat16)
    for head in range(groups):
        cut = slice(head * qk, (head + 1) * qk)
        kv_out[head, :, :width] = jnp.concatenate((first[:, cut], second[:, cut]), axis=1)
    loads[3].wait()
    head_v = v_hbm.shape[1] // groups
    for head in range(groups):
        cut = slice(head * head_v, (head + 1) * head_v)
        kv_out[head, :, width:] = jnp.dot(
            hid[...], wv[:, cut], preferred_element_type=jnp.float32
        ).astype(jnp.bfloat16)
    kv_all[me] = kv_out[plane]
    loads[4].wait()
    first = (project(wq1) * score_scale).astype(jnp.bfloat16)
    loads[5].wait()
    second = (project(wq2) * score_scale).astype(jnp.bfloat16)
    for head in range(groups):
        cut = slice(head * qk, (head + 1) * qk)
        q_out[head] = jnp.concatenate((first[:, cut], second[:, cut]), axis=1)
    q_all[plane] = q_out[plane]
    pl.semaphore_wait(barrier, groups - 1 + 3)

    def kv_copy(step):
        target = from_plane(step)
        return send(
            kv_out.at[target],
            kv_all.at[me],
            kv_send.at[step],
            kv_recv.at[plane],
            target * PLANE + spot,
            core,
        )

    def q_copy(step):
        target = from_plane(step)
        return send(
            q_out.at[target],
            q_all.at[plane],
            q_send.at[step],
            q_recv.at[plane],
            target * PLANE + spot,
            core,
        )

    def spread(step):
        block = from_plane(step) * PLANE + spot
        for sems, where in (((x_send, x_recv), x_spot), ((y_send, y_recv), y_spot)):
            copy = send(
                kv_all.at[block],
                kv_all.at[block],
                sems[0].at[step],
                sems[1].at[step],
                plane * PLANE + where,
                core,
            )
            copy.start()
            pending.append(copy)

    def arrived(recv_sem, block):
        pltpu.make_async_copy(kv_all.at[block], kv_all.at[block], recv_sem).wait()

    half = rows // 2

    def relay(step):
        x_block = from_plane(step) * PLANE + x_spot
        y_block = from_plane(step) * PLANE + y_spot
        for part, block, sem, where in (
            (0, x_block, x_recv, y_spot),
            (1, y_block, y_recv, x_spot),
        ):
            arrived(sem.at[step], block)
            piece = kv_all.at[block, pl.ds(part * half, half), :]
            copy = send(
                piece,
                piece,
                f_send.at[step, part],
                f_recv.at[step, part],
                plane * PLANE + where,
                core,
            )
            copy.start()
            pending.append(copy)

    kv_copy(1).start()
    spread(0)
    for step in range(2, groups):
        kv_copy(step).start()
        q_copy(step - 1).start()
    q_copy(groups - 1).start()
    loads[6].wait()
    wo_copy = send(wo.at[core], wo.at[core], wo_send, wo_recv, me, 1 - core)
    wo_copy.start()

    def forward_arrival(step):
        arrived(kv_recv.at[from_plane(step)], from_plane(step) * PLANE + spot)
        spread(step)

    def stage_ready(step):
        far = from_plane(step) * PLANE + (PLANE - 1 - spot)
        for part in range(2):
            piece = kv_all.at[far, pl.ds(part * half, half), :]
            pltpu.make_async_copy(piece, piece, f_recv.at[step, part]).wait()
        if step > 0:
            slot = q_all.at[from_plane(step)]
            pltpu.make_async_copy(slot, slot, q_recv.at[from_plane(step)]).wait()

    tile = ROW_TILE
    tiles = rows // tile
    chunk = PLANE * rows
    lane = lax.broadcasted_iota(jnp.int32, (tile, width), 1)
    lam = lam_ref[plane]
    gain = gain_ref[...]

    def pair_tile(group, key_group, part, diagonal):
        begin = pl.multiple_of(part * tile, tile)
        queries = q_all[group, pl.ds(begin, tile), :]
        zero = jnp.zeros_like(queries)
        both = jnp.concatenate(
            (jnp.where(lane < qk, queries, zero), jnp.where(lane >= qk, queries, zero)), axis=0
        )
        block = kv_all[pl.ds(key_group * PLANE, PLANE)].reshape(chunk, width + head_v)
        scores = lax.dot_general(
            both,
            block[:, :width],
            (((1,), (1,)), ((), ())),
            preferred_element_type=jnp.float32,
        )
        if diagonal:
            q_pos = spot * rows + begin + lax.rem(
                lax.broadcasted_iota(jnp.int32, (2 * tile, chunk), 0), tile
            )
            k_pos = lax.broadcasted_iota(jnp.int32, (2 * tile, chunk), 1)
            scores = jnp.where(k_pos <= q_pos, scores, masked_score)
        new_max = jnp.max(scores, axis=-1, keepdims=True)
        if not diagonal:
            running_max = max_all[group, part]
            new_max = jnp.maximum(running_max, new_max)
            rescale = jnp.exp2(running_max - new_max)
        weights = jnp.exp2(scores - new_max)
        new_sum = jnp.sum(weights, axis=-1, keepdims=True)
        accum = jnp.dot(
            weights.astype(jnp.bfloat16),
            block[:, width:],
            preferred_element_type=jnp.float32,
        )
        if not diagonal:
            new_sum = sum_all[group, part] * rescale + new_sum
            accum = acc_all[group, part] * rescale + accum
        max_all[group, part] = new_max
        sum_all[group, part] = new_sum
        acc_all[group, part] = accum

    def pair(group, key_group, diagonal):
        lax.fori_loop(
            0, tiles, lambda t, c: (pair_tile(group, key_group, t, diagonal), c)[1], 0
        )

    def meet(step, earlier):
        one, other = from_plane(step), from_plane(earlier)
        pair(jnp.maximum(one, other), jnp.minimum(one, other), False)

    def normed_copy(group):
        return send(
            n_out.at[group],
            n_all.at[core, plane],
            n_send.at[group],
            n_recv.at[plane],
            group * PLANE + spot,
            core,
        )

    def partner_copy(head):
        slot = n_all.at[core, head]
        return send(slot, slot, r_send.at[head], r_recv.at[head], me, 1 - core)

    def finish(group):
        def finish_tile(part, _):
            begin = pl.multiple_of(part * tile, tile)
            heads_out = acc_all[group, part] / sum_all[group, part]
            mixed = heads_out[:tile] - lam * heads_out[tile:]
            scale_rows = lax.rsqrt(jnp.mean(mixed * mixed, axis=-1, keepdims=True) + epsilon)
            normed = (mixed * scale_rows * gain).astype(jnp.bfloat16)
            n_out[group, pl.ds(begin, tile), :] = normed
            return 0

        lax.fori_loop(0, tiles, finish_tile, 0)

    def stage(step):
        stage_ready(step)
        pair(from_plane(step), from_plane(step), True)
        if step + 1 < groups:
            for earlier in range(step):
                meet(step, earlier)
        else:
            for earlier in list(range(1, step)) + [0]:
                meet(step, earlier)
                finish(from_plane(earlier))
                if earlier == 0:
                    n_all[core, plane] = n_out[plane]
                    partner_copy(plane).start()
                else:
                    normed_copy(from_plane(earlier)).start()

    for step in range(1, groups):
        forward_arrival(step)
        relay(step - 1)
        if step >= 2:
            stage(step - 2)
    relay(groups - 1)
    stage(groups - 2)
    stage(groups - 1)
    finish(from_plane(groups - 1))
    normed_copy(from_plane(groups - 1)).start()

    for step in range(1, groups):
        head = from_plane(step)
        slot = n_all.at[core, head]
        pltpu.make_async_copy(slot, slot, n_recv.at[head]).wait()
        partner_copy(head).start()
    wo_copy.wait_send()

    def out_tiles(tp_index, first_part):
        normed = jnp.concatenate([n_all[tp_index, head] for head in range(groups)], axis=1)

        def out_tile(index, _):
            columns = pl.ds(pl.multiple_of(index * OUT_TILE, OUT_TILE), OUT_TILE)
            part = jnp.dot(normed, wo[tp_index, :, columns], preferred_element_type=jnp.float32)
            part = part.astype(jnp.bfloat16)
            if not first_part:
                part = (part.astype(jnp.float32) + out_ref[:, columns].astype(jnp.float32)).astype(
                    jnp.bfloat16
                )
            out_ref[:, columns] = part
            return 0

        lax.fori_loop(0, out_ref.shape[1] // OUT_TILE, out_tile, 0)

    out_tiles(core, True)
    pltpu.make_async_copy(wo.at[1 - core], wo.at[1 - core], wo_recv).wait()
    for head in range(groups):
        slot = n_all.at[1 - core, head]
        pltpu.make_async_copy(slot, slot, r_recv.at[head]).wait()
    out_tiles(1 - core, False)

    for copy in pending:
        copy.wait_send()
    for step in range(1, groups):
        kv_copy(step).wait_send()
        q_copy(step).wait_send()
        normed_copy(from_plane(step)).wait_send()
    for head in range(groups):
        partner_copy(head).wait_send()


ROW_TILE = 256
OUT_TILE = 1024


def fused_shards(
    hidden_in, query_one, query_two, key_one, key_two, value_proj, lambdas, norm_gain, out_proj
):
    groups = lambdas.shape[0]
    rows, depth = hidden_in.shape
    head_qk = query_one.shape[1] // groups
    head_v = value_proj.shape[1] // groups
    width = 2 * head_qk
    blocks = groups * PLANE
    columns = out_proj.shape[1]
    score_scale = 1.75 * head_qk ** (-0.5) * math.log2(math.e)
    bf16 = jnp.bfloat16
    dma = pltpu.SemaphoreType.DMA
    hbm = pl.BlockSpec(memory_space=pl.ANY)
    vmem = pl.BlockSpec(memory_space=pltpu.VMEM)
    smem = pl.BlockSpec(memory_space=pltpu.SMEM)

    def body(*refs):
        fused_kernel(groups, score_scale, *refs)

    return pl.pallas_call(
        body,
        name="fused_attention",
        out_shape=jax.ShapeDtypeStruct((rows, columns), bf16),
        in_specs=[hbm] * 6 + [smem, vmem, hbm],
        out_specs=vmem,
        scratch_shapes=[
            pltpu.VMEM(hidden_in.shape, bf16),
            pltpu.VMEM(query_one.shape, bf16),
            pltpu.VMEM(query_two.shape, bf16),
            pltpu.VMEM(key_one.shape, bf16),
            pltpu.VMEM(key_two.shape, bf16),
            pltpu.VMEM(value_proj.shape, bf16),
            pltpu.VMEM((2,) + out_proj.shape, bf16),
            pltpu.VMEM((groups, rows, width + head_v), bf16),
            pltpu.VMEM((groups, rows, width), bf16),
            pltpu.VMEM((blocks, rows, width + head_v), bf16),
            pltpu.VMEM((groups, rows, width), bf16),
            pltpu.VMEM((groups, rows, head_v), bf16),
            pltpu.VMEM((2, groups, rows, head_v), bf16),
            pltpu.VMEM((groups, rows // ROW_TILE, 2 * ROW_TILE, 1), jnp.float32),
            pltpu.VMEM((groups, rows // ROW_TILE, 2 * ROW_TILE, 1), jnp.float32),
            pltpu.VMEM((groups, rows // ROW_TILE, 2 * ROW_TILE, head_v), jnp.float32),
            dma((7,)),
            dma,
            dma,
        ]
        + [dma((groups,))] * 8
        + [dma((groups, 2))] * 2
        + [dma((groups,))] * 4,
        compiler_params=pltpu.CompilerParams(
            collective_id=0, has_side_effects=True, vmem_limit_bytes=60 * 1024 * 1024
        ),
    )(
        hidden_in,
        query_one,
        query_two,
        key_one,
        key_two,
        value_proj,
        lambdas,
        norm_gain.reshape(1, head_v),
        out_proj,
    )


def solution(mesh):
    placed = (
        P("sp", None),
        P(None, "tp"),
        P(None, "tp"),
        P(None, "tp"),
        P(None, "tp"),
        P(None, "tp"),
        P("tp"),
        P(),
        P("tp", None),
    )

    def body(*args):
        groups = args[6].shape[0]
        split = groups * PLANE == mesh.shape["sp"] and mesh.shape["tp"] == 2
        return (fused_shards if split else shards)(*args)

    return jax.shard_map(
        body, mesh=mesh, in_specs=placed, out_specs=P("sp", None), check_vma=False
    )
```
